32 devices in a mesh: sp: 8 (over z, core), tp: 4 (over y, x).
Axes of the slice: x: 2, y: 2, z: 4, core: 2. Of those that a mesh axis runs over, the one named last changes fastest.
Arguments:
- outer_gate: bfloat16 [2048, 1024], P('sp', 'tp'), may hold values from -6 to 6
- inner_gate: bfloat16 [2048, 1024], P('sp', 'tp'), may hold values from -6 to 6
- values: bfloat16 [2048, 1024], P('sp', 'tp'), may hold values from -6 to 6
- conv_taps: bfloat16 [3, 1024], P(None, 'tp'), may hold values from -3.5 to 3.5
- document: int32 [2048], P('sp'), may hold values from 0 to 3, never falling along the last dimension, each value on 1 to 1024 neighbouring positions
- mix_proj: bfloat16 [1024, 2048], P('tp'), may hold values from -0.1875 to 0.1875
- stream: bfloat16 [2048, 2048], P('sp'), may hold values from -6 to 6
- norm_gain: float32 [2048], replicated, may hold values from 0.1 to 1.9
- routes: int32 [2048, 2], P('sp'), may hold values from 0 to 7, all different within a row; in each aligned block of 256 rows (0 to 255, 256 to 511, ...) at most 96 rows name the same one
- route_weight: float32 [2048, 2], P('sp'), may hold values from 0.25 to 1
- w_gate: bfloat16 [8, 2048, 4096], P('sp', None, 'tp'), may hold values from -0.125 to 0.125
- w_up: bfloat16 [8, 2048, 4096], P('sp', None, 'tp'), may hold values from -0.125 to 0.125
- w_down: bfloat16 [8, 4096, 2048], P('sp', 'tp'), may hold values from -0.09375 to 0.09375
Outputs:
- mixed: bfloat16 [2048, 2048], P('sp', 'tp')
The draws below stay inside these ranges and needn't reach their ends.
Inputs may be any that keep to these rules, and one draw needn't show every extreme that they name: Document numbers never fall along the sequence; each document holds 1 to 1024 consecutive tokens and one holds exactly that many. `routes`: each token names 2 different experts. Among the 256 tokens of one sp index no expert is named by more than 96 tokens, and in some sp index's tokens an expert is named by exactly 96.
All inputs are finite; a program needn't handle non-finite values.
Results may differ from the reference program's by a relative error of at most 0.014.
Values may be sent and summed in bfloat16 or wider, within the bound.
No kernel may reach another device: no remote copies, remote signals or barrier semaphores. Data moves between devices by JAX's collectives and lax.ppermute only.
A program may use at most 64 MiB of HBM per device.

```python
import math
import jax
import jax.numpy as jnp
import numpy as np
from jax import lax

D = 2048
DC = 1024
FFE = 4096
TOP = 2
TAPS = 3
T_SP = 256
TOKENS = 2048
EXPERTS = 8
CAP = 96
N_SP = 8
N_TP = 4


def shard_levels(stream_key, shape, shards, smallest, high):
    gain, own = 1.0, jax.random.fold_in(stream_key, 6)
    for dim, shards_of in shards:
        heights = jnp.exp(jax.random.uniform(jax.random.fold_in(own, dim), (shards_of,), jnp.float32, smallest / len(shards), high / len(shards)))
        gain = gain * jnp.repeat(heights, shape[dim] // shards_of).reshape([-1 if axis == dim else 1 for axis in range(len(shape))])
    return gain


def split_up(amount, total, most, slope):
    weights = [(1 << 20) // math.isqrt(standing ** slope) + 1 for standing in range(2, amount + 1)]
    spare, holding = total - most - (amount - 1), [1] * (amount - 1)
    while spare > 0:
        free = [i for i in range(amount - 1) if holding[i] < most]
        pool, remaining = sum([weights[i] for i in free]), spare
        for i in free:
            extra = min(most - holding[i], max(1, remaining * weights[i] // pool), spare)
            holding[i] = holding[i] + extra
            spare = spare - extra
    return np.array([most] + holding)


def ragged(stream_key, number_of, total, most, slope):
    if number_of == 2:
        one = jax.random.randint(stream_key, (), max(1, total - most), min(most, total - 1) + 1)
        return jnp.stack([one, total - one])
    lengths = jnp.asarray(split_up(number_of, total, most, slope), jnp.int32)
    pairs = (number_of - 1) // 2
    source_of, sink = lengths[1:1 + 2 * pairs:2], lengths[2:2 + 2 * pairs:2]
    slack = jnp.minimum(source_of - 1, most - sink)
    moved = jax.random.randint(jax.random.fold_in(stream_key, 1), (pairs,), 0, 1 << 20) % (slack + 1)
    lengths = lengths.at[1:1 + 2 * pairs:2].set(source_of - moved).at[2:2 + 2 * pairs:2].set(sink + moved)
    return lengths[jax.random.permutation(jax.random.fold_in(stream_key, 2), number_of)]


def assign_block(stream_key, own, number, rows, count, top, most, slope):
    ranking = jax.random.permutation(stream_key, count)
    packed, usual = load_shares(count, rows * top, most, slope, True), load_shares(count, rows * top, most, slope, False)
    places = jnp.arange(count)

    def named(lengths, turn):
        used = int((lengths > 0).sum())
        fixed = max(1, used // 4)
        moved = fixed + (places - fixed + turn * (used - fixed)) % max(1, count - fixed)
        return jnp.zeros((count,), jnp.int32).at[ranking[jnp.where(places < fixed, places, moved)]].set(jnp.asarray(lengths, jnp.int32))

    lengths = jnp.where(number % 4 == 0, named(packed, number // 4), named(usual, number - number // 4 - 1))
    mixed = jax.random.permutation(jax.random.fold_in(own, 3), count)
    source_of, taker = mixed[0:count // 2 * 2:2], mixed[1:count // 2 * 2:2]
    margin = jnp.minimum(lengths[source_of] - 1, most - lengths[taker]) // 2
    margin = jnp.where((source_of == ranking[0]) | (taker == ranking[0]) | (lengths[taker] == 0), 0, jnp.maximum(margin, 0))
    moved = jax.random.randint(jax.random.fold_in(own, 4), (count // 2,), 0, 1 << 20) % (margin + 1)
    lengths = lengths.at[source_of].add(-moved).at[taker].add(moved)
    items = jnp.searchsorted(jnp.cumsum(lengths), jnp.arange(rows * top), side="right").astype(jnp.int32)
    listing = items.reshape(top, rows).T
    listing = listing[jax.random.permutation(jax.random.fold_in(own, 1), rows)]
    turn = jax.random.randint(jax.random.fold_in(own, 2), (rows, 1), 0, top)
    return jnp.take_along_axis(listing, (jnp.arange(top)[None, :] + turn) % top, axis=1)


def load_shares(amount, total, bound, lean, full):
    weights = [(1 << 20) // math.isqrt(rank ** lean) + 1 for rank in range(1, amount + 1)]
    largest = bound if full else min(bound, max(-(-total // amount), total * weights[0] // sum(weights)))
    least = 1 if total - largest >= amount - 1 else 0
    counts, rest = [largest] + [least] * (amount - 1), total - largest - least * (amount - 1)
    while rest > 0:
        candidates = [i for i in range(1, amount) if counts[i] < largest] or [i for i in range(1, amount) if counts[i] < bound]
        pool, budget = sum([weights[i] for i in candidates]), rest
        for i in candidates:
            extra = min(bound - counts[i], max(1, budget * weights[i] // pool), rest)
            counts[i] = counts[i] + extra
            rest = rest - extra
    return np.array(counts)


def centred(stream_key, extent, deviation, reach, cuts=(), kind=jnp.bfloat16):
    factor_of = shard_levels(stream_key, extent, cuts, -0.22, 0.18) if cuts else 1.0
    drawn = jax.random.normal(stream_key, extent, jnp.float32) * deviation * factor_of
    return jnp.minimum(jnp.maximum(drawn, -reach), reach).astype(kind)


def setup_inputs(seed: int = 0) -> dict:
    key_list = jax.random.split(jax.random.key(seed), 14)
    outer_gate = centred(key_list[0], (TOKENS, DC), 1.0, 6.0, ((0, 8), (1, 4)))
    inner_gate = centred(key_list[1], (TOKENS, DC), 1.0, 6.0, ((0, 8), (1, 4)))
    values = centred(key_list[2], (TOKENS, DC), 1.0, 6.0, ((0, 8), (1, 4)))
    conv_taps = centred(key_list[3], (TAPS, DC), TAPS ** -0.5, 3.5, ((1, 4),))
    document = jnp.searchsorted(jnp.cumsum(ragged(key_list[4], N_SP // 2, TOKENS, 4 * T_SP, 1)), jnp.arange(TOKENS), side="right").astype(jnp.int32)
    mix_proj = centred(key_list[5], (DC, D), DC ** -0.5, 0.1875, ((0, 4),))
    stream = centred(key_list[6], (TOKENS, D), 1.0, 6.0, ((0, 8),))
    norm_gain = jnp.clip(1.0 + 0.18 * jax.random.normal(key_list[7], (D,), jnp.float32), 0.1, 1.9)
    routes_keys = jax.random.split(jax.random.fold_in(key_list[8], 1), TOKENS // T_SP)
    routes_turns = jax.random.permutation(jax.random.fold_in(key_list[8], 3), TOKENS // T_SP)
    routes = jax.vmap(lambda own, number: assign_block(jax.random.fold_in(key_list[8], 2), own, number, T_SP, EXPERTS, TOP, CAP, 2))(routes_keys, routes_turns).reshape((TOKENS, TOP))
    route_weight = jnp.clip(0.25 + 0.75 * jax.random.uniform(key_list[9], (TOKENS, TOP), jnp.float32) ** shard_levels(key_list[9], (TOKENS, TOP), ((0, 8),), -0.2, 0.2), 0.25, 1.0)
    w_gate = centred(key_list[10], (EXPERTS, D, FFE), D ** -0.5, 0.125, ((0, 8), (2, 4)))
    w_up = centred(key_list[11], (EXPERTS, D, FFE), D ** -0.5, 0.125, ((0, 8), (2, 4)))
    w_down = centred(key_list[12], (EXPERTS, FFE, D), FFE ** -0.5, 0.09375, ((0, 8), (1, 4)))
    return {"outer_gate": outer_gate, "inner_gate": inner_gate, "values": values, "conv_taps": conv_taps, "document": document, "mix_proj": mix_proj, "stream": stream, "norm_gain": norm_gain, "routes": routes, "route_weight": route_weight, "w_gate": w_gate, "w_up": w_up, "w_down": w_down}


def rounded(value):
    held = lax.optimization_barrier(value.astype(jnp.bfloat16))
    return held.astype(jnp.float32)

def reference(outer_gate, inner_gate, values, conv_taps, document, mix_proj, stream, norm_gain, routes, route_weight, w_gate, w_up, w_down):
    length = stream.shape[0]
    product = inner_gate.astype(jnp.float32) * values.astype(jnp.float32)
    kernel = conv_taps.astype(jnp.float32)
    conv = kernel[2] * product
    for back in (1, 2):
        shifted = jnp.pad(product, ((back, 0), (0, 0)))[:length]
        earlier = jnp.pad(document, (back, 0), constant_values=-1)[:length]
        same = (earlier == document)[:, None]
        conv = conv + kernel[2 - back] * jnp.where(same, shifted, 0.0)
    gated = (outer_gate.astype(jnp.float32) * conv).astype(jnp.bfloat16)
    group_width = DC // N_TP
    branch = jnp.zeros((length, D), jnp.float32)
    for group in range(N_TP):
        lower = group * group_width
        partial_value = jnp.dot(gated[:, lower:lower + group_width], mix_proj[lower:lower + group_width], preferred_element_type=jnp.float32)
        branch = branch + rounded(partial_value)
    hidden_state = stream.astype(jnp.float32) + branch
    scale = lax.rsqrt(lax.optimization_barrier(jnp.mean(hidden_state * hidden_state, axis=-1, keepdims=True)) + 1e-06)
    normed = (hidden_state * scale * norm_gain).astype(jnp.bfloat16)
    flat_expert = routes.reshape(-1).astype(jnp.int32)
    count = flat_expert.shape[0]
    flat_token = jnp.arange(count, dtype=jnp.int32) // TOP
    flat_weight = route_weight.reshape(-1)
    order_key = jnp.arange(count, dtype=jnp.int32)
    limit = N_SP * CAP
    hidden_width = FFE // N_TP

    def per_expert(carry, expert):
        keyed = jnp.where(flat_expert == expert, order_key, count)
        chosen = jnp.argsort(keyed, stable=True)[:limit].astype(jnp.int32)
        valid = jnp.take(keyed, chosen) < count
        token_index = jnp.take(flat_token, chosen)
        taken = jnp.take(normed, token_index, axis=0)
        gate = jnp.dot(taken, w_gate[expert], preferred_element_type=jnp.float32)
        upper = jnp.dot(taken, w_up[expert], preferred_element_type=jnp.float32)
        act = (jax.nn.silu(gate) * upper).astype(jnp.bfloat16)
        down = w_down[expert]
        total = jnp.zeros((limit, D), jnp.float32)
        for group in range(N_TP):
            lower = group * hidden_width
            partial_value = jnp.dot(act[:, lower:lower + hidden_width], down[lower:lower + hidden_width], preferred_element_type=jnp.float32)
            total = total + rounded(partial_value)
        expert_out = rounded(total)
        weight = jnp.where(valid, jnp.take(flat_weight, chosen), 0.0)
        carry = carry.at[token_index].add(weight[:, None] * expert_out)
        return (carry, None)
    combined, _ = lax.scan(per_expert, jnp.zeros((length, D), jnp.float32), jnp.arange(EXPERTS, dtype=jnp.int32))
    return (hidden_state + combined).astype(jnp.bfloat16)
```

```python
import functools

import jax
import jax.numpy as jnp
from jax import lax
from jax.experimental import pallas as pl
from jax.experimental.pallas import tpu as pltpu
from jax.sharding import PartitionSpec as P


BF16 = jnp.bfloat16
F32 = jnp.float32


def swap(value, axis, distance):
    count = lax.axis_size(axis)
    return lax.ppermute(value, axis, [(i, i ^ distance) for i in range(count)])


def gathered(piece, bits):
    low = piece[None]
    for bit in bits[:-1]:
        low = jnp.concatenate([low, swap(low, "tp", bit)], axis=0)
    return low, swap(low, "tp", bits[-1])


def offsets(bits):
    order = [0]
    for bit in bits:
        order = order + [other ^ bit for other in order]
    return order


def scatter_plan(bits):
    keep = [0]
    for bit in reversed(bits[1:]):
        keep = [other ^ bit for other in keep] + keep
    return [other ^ bits[0] for other in keep], keep


def scattered(send, keep, bits):
    for index, bit in enumerate(bits):
        total = keep.astype(F32) + swap(send, "tp", bit).astype(F32)
        if index + 1 == len(bits):
            return total[0].astype(BF16)
        half = total.shape[0] // 2
        send, keep = total[:half].astype(BF16), total[half:]


def expert_kernel(
    place, inverse_gain, low_a, high_a, low_b, high_b, w_gate, w_up, w_down,
    send_a, keep_a, send_b, keep_b, rows, scale, act, *, bits, steps, block, epsilon,
):
    step = pl.program_id(0)
    own = place[0]
    count, total_rows, width = rows.shape
    half_rows = total_rows // 2
    half = count // 2

    @pl.when(step == 0)
    def _():
        square = jnp.zeros((total_rows, 1), F32)
        for start, order, low, high in (
            (0, offsets(bits), low_a, high_a),
            (half_rows, offsets(bits[::-1]), low_b, high_b),
        ):
            for index, offset in enumerate(order):
                source = low if index < half else high
                rows[own ^ offset, start : start + half_rows, :] = source[index % half]
        for index in range(count):
            value = rows[index].astype(F32) * inverse_gain[index]
            square = square + jnp.sum(value * value, axis=1, keepdims=True)
        scale[...] = jnp.broadcast_to(
            lax.rsqrt(square / (count * width) + epsilon), scale.shape
        )

    for index in range(steps):
        @pl.when(step == index)
        def _():
            gate = jnp.zeros((total_rows, block), F32)
            upper = jnp.zeros((total_rows, block), F32)
            for part in range(count):
                piece = rows[part]
                span = slice(part * width, (part + 1) * width)
                gate = gate + jnp.dot(piece, w_gate[0, span, :], preferred_element_type=F32)
                upper = upper + jnp.dot(piece, w_up[0, span, :], preferred_element_type=F32)
            factor = scale[:, :1]
            gate = gate * factor
            upper = upper * factor
            act[:, index * block : (index + 1) * block] = (
                gate / (1.0 + jnp.exp(-gate)) * upper
            ).astype(BF16)

    for start, order, send, keep in (
        (0, scatter_plan(bits), send_a, keep_a),
        (half_rows, scatter_plan(bits[::-1]), send_b, keep_b),
    ):
        for index in range(count):
            target = send if index < half else keep
            offset = (order[0] + order[1])[index]

            @pl.when(step == steps + offset)
            def _():
                target[index % half] = jnp.dot(
                    act[start : start + half_rows], w_down[0], preferred_element_type=F32
                ).astype(BF16)


def run_experts(place, inverse_gain, flow_a, flow_b, w_gate, w_up, w_down, bits):
    half, half_rows, width = flow_a[0].shape
    count = 2 * half
    features, hidden = w_gate.shape[1:]
    block = min(256, hidden)
    steps = hidden // block
    whole = lambda shape: pl.BlockSpec(shape, lambda i, p: (0,) * len(shape))
    piece_spec = whole((half, half_rows, width))
    into = lambda i, p: (0, 0, jnp.minimum(i, steps - 1))
    down = lambda i, p: (0, 0, p[0] ^ jnp.maximum(i - steps, 0))
    piece_type = jax.ShapeDtypeStruct((half, half_rows, width), BF16)
    return pl.pallas_call(
        functools.partial(expert_kernel, bits=bits, steps=steps, block=block, epsilon=1e-06),
        grid_spec=pltpu.PrefetchScalarGridSpec(
            num_scalar_prefetch=1,
            grid=(steps + count,),
            in_specs=[
                whole((count, 1, width)),
                piece_spec, piece_spec, piece_spec, piece_spec,
                pl.BlockSpec((1, features, block), into),
                pl.BlockSpec((1, features, block), into),
                pl.BlockSpec((1, hidden, width), down),
            ],
            out_specs=[piece_spec] * 4,
            scratch_shapes=[
                pltpu.VMEM((count, 2 * half_rows, width), BF16),
                pltpu.VMEM((2 * half_rows, 128), F32),
                pltpu.VMEM((2 * half_rows, hidden), BF16),
            ],
        ),
        out_shape=[piece_type] * 4,
        cost_estimate=pl.CostEstimate(
            flops=2 * 2 * half_rows * features * hidden * 3,
            bytes_accessed=6 * features * hidden,
            transcendentals=2 * half_rows * hidden,
        ),
        name="experts",
    )(place, inverse_gain, *flow_a, *flow_b, w_gate, w_up, w_down)


def body(
    outer_gate,
    inner_gate,
    values,
    conv_taps,
    document,
    mix_proj,
    stream,
    norm_gain,
    routes,
    route_weight,
    w_gate,
    w_up,
    w_down,
):
    length, features = stream.shape
    groups = lax.axis_size("sp")
    parts = lax.axis_size("tp")
    capacity = 3 * length // groups
    chosen_count = routes.shape[1]
    width = features // parts
    chips = groups // 2
    own = lax.axis_index("tp")
    place = lax.axis_index("sp")
    column = own * width
    bits = [1 << shift for shift in range(parts.bit_length() - 1)]

    product = inner_gate.astype(F32) * values.astype(F32)
    doc_float = document.astype(F32)
    rim = jnp.concatenate(
        [product[-2:], jnp.broadcast_to(doc_float[-2:, None], (2, 128))], axis=1
    )
    rim = lax.ppermute(rim, "sp", [(i, i + 1) for i in range(groups - 1)])
    channels = product.shape[1]
    first = place == 0
    rim_docs = jnp.where(first, -1.0, rim[:, channels])
    padded_values = jnp.concatenate([rim[:, :channels], product], axis=0)
    padded_docs = jnp.concatenate([rim_docs, doc_float], axis=0)
    kernel = conv_taps.astype(F32)
    conv = kernel[2] * product
    for back in (1, 2):
        offset = 2 - back
        same = (padded_docs[offset : offset + length] == doc_float)[:, None]
        conv = conv + kernel[offset] * jnp.where(same, padded_values[offset : offset + length], 0.0)
    gated = (outer_gate.astype(F32) * conv).astype(BF16)

    flat_expert = routes.reshape(-1)
    picks = (flat_expert[:, None] == jnp.arange(groups, dtype=jnp.int32)[None, :]).astype(jnp.int32)
    ranking = jnp.sum((jnp.cumsum(picks, axis=0) - 1) * picks, axis=1)
    relative = flat_expert ^ place
    position = ((relative % 2) * chips + relative // 2) * capacity + ranking
    position = position.reshape(length, chosen_count)
    slots = jnp.arange(groups * capacity, dtype=jnp.int32)
    chosen = [position[:, k][None, :] == slots[:, None] for k in range(chosen_count)]
    spread = functools.reduce(jnp.logical_or, chosen).astype(BF16)

    hidden = lax.dynamic_slice_in_dim(stream, column, width, 1).astype(F32)
    for distance in range(parts):
        target = (own ^ distance) * width
        part = jnp.dot(
            gated,
            lax.dynamic_slice_in_dim(mix_proj, target, width, 1),
            preferred_element_type=F32,
        ).astype(BF16)
        hidden = hidden + (swap(part, "tp", distance) if distance else part).astype(F32)
    gain = lax.dynamic_slice_in_dim(norm_gain, column, width, 0)
    scaled = (hidden * gain).astype(BF16)
    outgoing = jnp.dot(spread, scaled, preferred_element_type=F32).astype(BF16)
    outgoing = outgoing.reshape(2, chips, capacity, width)
    mate = swap(outgoing[1], "sp", 1)
    rows_for = [
        jnp.concatenate([outgoing[0, d], mate[d]], axis=0) for d in range(chips)
    ]
    arrived = [swap(rows_for[d], "sp", 2 * d) if d else rows_for[d] for d in range(chips)]

    inverse_gain = (1.0 / norm_gain).reshape(parts, 1, width)
    tag = own.astype(jnp.int32).reshape(1)
    quarter = chips // 4
    orders = [[0, 2], [1, 3]]
    returned = [None] * chips
    for pair in orders:
        lists = [list(range(q * quarter, (q + 1) * quarter)) for q in pair]
        flows = [jnp.concatenate([arrived[d] for d in ds], axis=0) for ds in lists]
        flow_bits = [bits, bits[::-1]]
        lows = [gathered(flow, b) for flow, b in zip(flows, flow_bits)]
        send_a, keep_a, send_b, keep_b = run_experts(
            tag, inverse_gain, lows[0], lows[1], w_gate, w_up, w_down, bits
        )
        for ds, send, keep, b in ((lists[0], send_a, keep_a, bits), (lists[1], send_b, keep_b, bits[::-1])):
            total = scattered(send, keep, b).reshape(len(ds), 2 * capacity, width)
            for index, d in enumerate(ds):
                back = total[index]
                returned[d] = swap(back, "sp", 2 * d) if d else back
    mine = jnp.concatenate([block[:capacity] for block in returned], axis=0)
    other = jnp.concatenate([block[capacity:] for block in returned], axis=0)
    landed = jnp.concatenate([mine, swap(other, "sp", 1)], axis=0)
    total = hidden
    for k in range(chosen_count):
        fetched = lax.dot_general(
            chosen[k].astype(BF16), landed, (((0,), (0,)), ((), ())), preferred_element_type=F32
        )
        total = total + fetched * route_weight[:, k][:, None]
    return total.astype(BF16)


def solution(mesh):
    return jax.shard_map(
        body,
        mesh=mesh,
        in_specs=(
            P("sp", "tp"),
            P("sp", "tp"),
            P("sp", "tp"),
            P(None, "tp"),
            P("sp"),
            P("tp", None),
            P("sp", None),
            P(),
            P("sp", None),
            P("sp", None),
            P("sp", None, "tp"),
            P("sp", None, "tp"),
            P("sp", "tp", None),
        ),
        out_specs=P("sp", "tp"),
        check_vma=False,
    )
```

```python
import functools

import jax
import jax.numpy as jnp
from jax import lax
from jax.experimental import pallas as pl
from jax.experimental.pallas import tpu as pltpu
from jax.sharding import PartitionSpec as P


BF16 = jnp.bfloat16
F32 = jnp.float32
VMEM_LIMIT = 12 * 2**20
GATHERS = ("xy", "xy", "yx", "yx")
SCATTERS = ("yx", "yx", "xy", "xy")


def swap(value, axis, distance):
    count = lax.axis_size(axis)
    return lax.ppermute(value, axis, [(i, i ^ distance) for i in range(count)])


def gathered(own, bits):
    pieces = [own]
    for _ in range(1, 1 << len(bits)):
        pieces.append(None)
    known = [0]
    for bit in bits:
        for offset in list(known):
            pieces[offset ^ bit] = swap(pieces[offset], "tp", bit)
            known.append(offset ^ bit)
    return pieces


def scattered(pieces, bits):
    sums = [piece.astype(F32) for piece in pieces]
    waiting = list(range(len(pieces)))
    for bit in bits:
        for offset in [other for other in waiting if other & bit]:
            outgoing = sums[offset].astype(BF16)
            moved = swap(outgoing, "tp", bit)
            rest = offset ^ bit
            sums[rest] = sums[rest] + moved.astype(F32)
        waiting = [other for other in waiting if not other & bit]
    return sums[0].astype(BF16)


def start_kernel(
    outer, inner, values, taps, document, mix_proj, local, edge, head, first_outer, *refs, count
):
    blocks = refs[: count + 1]
    fetched, kernel_rows, ids, shifted, seen, semaphores = refs[count + 1 :]
    length, channels = outer.shape
    half, width = blocks[0].shape
    core, own = lax.axis_index("sp") % 2, lax.axis_index("tp")
    plan = [
        (document, ids), (inner, fetched.at[0]), (values, fetched.at[1]), (outer, fetched.at[2]),
        (taps, kernel_rows),
    ]
    for index, block in enumerate(blocks):
        which, distance = (core, index) if index < count else (1 - core, 0)
        row = pl.multiple_of(which * half, half)
        column = pl.multiple_of((own ^ distance) * width, width)
        plan.append((mix_proj.at[pl.ds(row, half), pl.ds(column, width)], block))
    copies = [
        pltpu.make_async_copy(source, target, semaphores.at[place])
        for place, (source, target) in enumerate(plan)
    ]
    for copy in copies:
        copy.start()
    copies[0].wait()
    lanes = max(channels, 128)
    docs = jnp.broadcast_to(ids[...].astype(F32), (lanes, length)).T[:, :channels]
    seen[:8, :] = jnp.full((8, channels), -1.0, F32)
    seen[8:, :] = docs
    shifted[:8, :] = jnp.zeros((8, channels), F32)
    for copy in copies[1:5]:
        copy.wait()
    kernel = kernel_rows[...].astype(F32)
    product = fetched[0].astype(F32) * fetched[1].astype(F32)
    shifted[8:, :] = product
    conv = kernel[2:3] * product
    for back in (1, 2):
        window = slice(8 - back, 8 - back + length)
        same = seen[window, :] == docs
        conv = conv + kernel[2 - back : 3 - back] * jnp.where(same, shifted[window, :], 0.0)
    gate = fetched[2].astype(F32)
    local[...] = gate * conv
    first_outer[...] = gate[:8]
    head[...] = docs[:8]
    edge[:, :channels] = product[length - 8 :]
    edge[:, channels:] = docs[length - 8 :]
    for copy in copies[5:]:
        copy.wait()


def slot_kernel(routes, weights, spread, first, second, columns, *, groups, capacity):
    rows, length = first.shape
    place = lax.axis_index("sp")
    expert = lax.broadcasted_iota(jnp.int32, (groups, length), 0)
    named = [(routes[k : k + 1, :] == expert).astype(F32) for k in range(2)]
    earlier = lax.broadcasted_iota(jnp.int32, (length, length), 0)
    later = lax.broadcasted_iota(jnp.int32, (length, length), 1)
    before = jnp.dot(
        (named[0] + named[1]).astype(BF16),
        (earlier < later).astype(F32).astype(BF16),
        preferred_element_type=F32,
    )
    slot = lax.broadcasted_iota(jnp.int32, (rows, length), 0)
    total = jnp.zeros((rows, length), F32)
    for k, target in enumerate((first, second)):
        rank = jnp.sum(before * named[k], axis=0, keepdims=True).astype(jnp.int32)
        relative = routes[k : k + 1, :] ^ place
        block = (relative & 1) * (groups // 2) + (relative >> 1)
        chosen = (slot == block * capacity + rank).astype(F32)
        target[...] = chosen.astype(BF16)
        total = total + chosen
        columns[k] = jnp.broadcast_to(weights[k : k + 1, :], (128, length)).T
    spread[...] = total.astype(BF16)


def combine_kernel(total, first, second, columns, landed, output, *, start):
    rows = landed.shape[0]
    result = total[...]
    for k, chosen in enumerate((first, second)):
        fetched = lax.dot_general(
            chosen[start : start + rows, :],
            landed[...],
            (((0,), (0,)), ((), ())),
            preferred_element_type=F32,
        )
        result = result + fetched * columns[k][:, :1]
    output[...] = result.astype(output.dtype)


def edge_kernel(local, rim, head, first_outer, taps, gated):
    channels = local.shape[1]
    kernel = taps[...].astype(F32)
    older, newer = rim[6:7, :channels], rim[7:8, :channels]
    older_doc, newer_doc = rim[6:7, channels:], rim[7:8, channels:]
    doc = head[...]
    row = lax.broadcasted_iota(jnp.int32, doc.shape, 0)
    one = kernel[1:2] * jnp.where((row == 0) & (newer_doc == doc), newer, 0.0)
    two = kernel[0:1] * (
        jnp.where((row == 0) & (older_doc == doc), older, 0.0)
        + jnp.where((row == 1) & (newer_doc == doc), newer, 0.0)
    )
    gated[...] = local[...].astype(BF16)
    first = local[:16]
    fixed = jnp.concatenate([first[:8] + first_outer[...] * (one + two), first[8:]], axis=0)
    gated[:16, :] = fixed.astype(BF16)


def mix_kernel(stream, gain, spread, own_rest, rest, *refs, count):
    pieces, mine = refs[:count], refs[count : 2 * count]
    hidden, kept, given, weight = refs[2 * count :]
    half, width = own_rest.shape
    core = lax.axis_index("sp") % 2
    here = pl.ds(pl.multiple_of(core * half, half), half)
    there = pl.ds(pl.multiple_of((1 - core) * half, half), half)
    span = pl.ds(pl.multiple_of(lax.axis_index("tp") * width, width), width)
    total = stream[:, span].astype(F32)
    for index in range(count):
        weight[index, here, :] = mine[index][...]
        weight[index, there, :] = rest[index - 1] if index else own_rest[...]
        total = total + jnp.dot(
            pieces[index][...], weight[index], preferred_element_type=F32
        )
    hidden[...] = total
    scaled = (total * gain[:, span]).astype(BF16)
    rows = kept.shape[0]
    kept[...] = jnp.dot(spread[:rows], scaled, preferred_element_type=F32).astype(BF16)
    given[...] = jnp.dot(spread[rows:], scaled, preferred_element_type=F32).astype(BF16)


def expert_kernel(norm_gain, w_gate, w_up, w_down, *refs, count, block, epsilon):
    pieces, outputs, act = refs[:count], refs[count : 2 * count], refs[2 * count]
    own = lax.axis_index("tp")
    rows, width = pieces[0].shape
    spans = [
        pl.ds(pl.multiple_of((own ^ offset) * width, width), width) for offset in range(count)
    ]
    square = jnp.zeros((rows, 1), F32)
    for piece, span in zip(pieces, spans):
        value = piece[...].astype(F32) / norm_gain[:, span]
        square = square + jnp.sum(value * value, axis=1, keepdims=True)
    factor = lax.rsqrt(square / (count * width) + epsilon)
    for column in range(0, act.shape[1], block):
        both = []
        for table in (w_gate, w_up):
            total = jnp.zeros((rows, block), F32)
            for piece, span in zip(pieces, spans):
                total = total + jnp.dot(
                    piece[...],
                    table[0, span, column : column + block],
                    preferred_element_type=F32,
                )
            both.append(total * factor)
        gate, upper = both
        act[:, column : column + block] = (gate / (1.0 + jnp.exp(-gate)) * upper).astype(BF16)
    for output, span in zip(outputs, spans):
        output[...] = jnp.dot(
            act[...], w_down[0, :, span], preferred_element_type=F32
        ).astype(BF16)


def vmem_shape(shape, dtype):
    return pltpu.VMEM(tuple(shape), dtype)


def local_call(kernel, out_shape, scratch_shapes, arrays, flops=0):
    vmem = pl.BlockSpec(memory_space=pltpu.VMEM)
    return pl.pallas_call(
        kernel,
        in_specs=[vmem] * len(arrays),
        out_specs=[vmem] * len(out_shape) if isinstance(out_shape, list) else vmem,
        out_shape=out_shape,
        scratch_shapes=scratch_shapes,
        cost_estimate=pl.CostEstimate(flops=flops, bytes_accessed=0, transcendentals=0),
        compiler_params=pltpu.CompilerParams(vmem_limit_bytes=VMEM_LIMIT),
    )(*arrays)


def body(
    outer_gate,
    inner_gate,
    values,
    conv_taps,
    document,
    mix_proj,
    stream,
    norm_gain,
    routes,
    route_weight,
    w_gate,
    w_up,
    w_down,
):
    length, features = stream.shape
    groups = lax.axis_size("sp")
    parts = lax.axis_size("tp")
    capacity = 3 * length // groups
    chosen_count = routes.shape[1]
    width = features // parts
    chips = groups // 2
    channels = values.shape[1]
    bits = [1 << shift for shift in range(parts.bit_length() - 1)]

    half = channels // 2
    head_shape = vmem_shape((8, channels), F32)
    vmem = pl.BlockSpec(memory_space=pltpu.VMEM)
    local, edge, head, first_outer, *mine = pl.pallas_call(
        functools.partial(start_kernel, count=parts),
        in_specs=[pl.BlockSpec(memory_space=pltpu.HBM)] * 6,
        out_specs=[vmem] * (5 + parts),
        out_shape=[
            vmem_shape((length, channels), F32),
            vmem_shape((8, 2 * channels), F32),
            head_shape,
            head_shape,
        ]
        + [vmem_shape((half, width), BF16)] * (parts + 1),
        scratch_shapes=[
            pltpu.VMEM((3, length, channels), BF16),
            pltpu.VMEM(conv_taps.shape, BF16),
            pltpu.VMEM((1, length), jnp.int32),
            pltpu.VMEM((length + 8, channels), F32),
            pltpu.VMEM((length + 8, channels), F32),
            pltpu.SemaphoreType.DMA((6 + parts,)),
        ],
        compiler_params=pltpu.CompilerParams(vmem_limit_bytes=VMEM_LIMIT),
        cost_estimate=pl.CostEstimate(flops=10**10, bytes_accessed=1, transcendentals=0),
        name="start",
    )(
        *[
            pltpu.with_memory_space_constraint(array, pltpu.HBM)
            for array in (
                outer_gate, inner_gate, values, conv_taps, document.reshape(1, length), mix_proj
            )
        ],
    )
    own_rest = mine.pop()
    for distance in range(1, parts):
        mine[distance] = swap(mine[distance], "tp", distance)
    rim = lax.ppermute(edge, "sp", [(i, i + 1) for i in range(groups - 1)])
    rest = jnp.stack(mine[1:])
    rest = swap(rest, "sp", 1)
    gated = local_call(
        edge_kernel,
        vmem_shape((length, channels), BF16),
        [],
        [local, rim, head, first_outer, conv_taps],
    )
    pieces = [gated]
    for distance in range(1, parts):
        pieces.append(swap(gated, "tp", distance))

    rows = groups * capacity
    select = vmem_shape((rows, length), BF16)
    spread, first, second, columns = local_call(
        functools.partial(slot_kernel, groups=groups, capacity=capacity),
        [select, select, select, vmem_shape((chosen_count, length, 128), F32)],
        [],
        [routes.T, route_weight.T],
    )

    half_rows = chips * capacity
    hidden, kept, given = local_call(
        functools.partial(mix_kernel, count=parts),
        [
            vmem_shape((length, width), F32),
            vmem_shape((half_rows, width), BF16),
            vmem_shape((half_rows, width), BF16),
        ],
        [pltpu.VMEM((parts, channels, width), BF16)],
        [stream, norm_gain.reshape(1, features), spread, own_rest, rest, *pieces, *mine],
    )
    kept = kept.reshape(chips, capacity, width)
    mate = swap(given, "sp", 1).reshape(chips, capacity, width)

    quarter = chips // 4
    returned = [None] * chips
    gather_bits = [bits if order == "xy" else bits[::-1] for order in GATHERS]
    scatter_bits = [bits if order == "xy" else bits[::-1] for order in SCATTERS]
    for flow in range(4):
        members = list(range(flow * quarter, (flow + 1) * quarter))
        arrived = []
        for d in members:
            rows = jnp.concatenate([kept[d], mate[d]], axis=0)
            if d:
                rows = swap(rows, "sp", 2 * d)
            arrived.append(rows)
        pieces = gathered(jnp.concatenate(arrived, axis=0), gather_bits[flow])
        flow_rows = pieces[0].shape[0]
        outputs = local_call(
            functools.partial(
                expert_kernel,
                count=parts,
                block=min(512, w_gate.shape[2]),
                epsilon=1e-06,
            ),
            [vmem_shape((flow_rows, width), BF16)] * parts,
            [pltpu.VMEM((flow_rows, w_gate.shape[2]), BF16)],
            [norm_gain.reshape(1, features), w_gate, w_up, w_down, *pieces],
            6 * flow_rows * features * w_gate.shape[2],
        )
        total = scattered(outputs, scatter_bits[flow])
        total = total.reshape(len(members), 2 * capacity, width)
        for index, d in enumerate(members):
            back = total[index]
            if d:
                back = swap(back, "sp", 2 * d)
            returned[d] = back
    here = jnp.concatenate([block[:capacity] for block in returned], axis=0)
    there = jnp.concatenate([block[capacity:] for block in returned], axis=0)
    there = swap(there, "sp", 1)
    total = hidden
    result = jax.ShapeDtypeStruct((length, width), BF16)
    for landed, start, shape in ((here, 0, jax.ShapeDtypeStruct(hidden.shape, F32)), (there, half_rows, result)):
        total = local_call(
            functools.partial(combine_kernel, start=start),
            shape,
            [],
            [total, first, second, columns, landed],
        )
    return total


def solution(mesh):
    return jax.shard_map(
        body,
        mesh=mesh,
        in_specs=(
            P("sp", "tp"),
            P("sp", "tp"),
            P("sp", "tp"),
            P(None, "tp"),
            P("sp"),
            P("tp", None),
            P("sp", None),
            P(),
            P("sp", None),
            P("sp", None),
            P("sp", None, "tp"),
            P("sp", None, "tp"),
            P("sp", "tp", None),
        ),
        out_specs=P("sp", "tp"),
        check_vma=False,
    )
```

```python
import functools

import jax
import jax.numpy as jnp
from jax import lax
from jax.experimental import pallas as pl
from jax.experimental.pallas import tpu as pltpu
from jax.sharding import PartitionSpec as P


BF16 = jnp.bfloat16
F32 = jnp.float32
VMEM_LIMIT = 12 * 2**20
GATHERS = ("yx", "yx", "yx", "xy")
SCATTERS = ("yx", "xy", "yx", "yx")


def swap(value, axis, distance):
    count = lax.axis_size(axis)
    return lax.ppermute(value, axis, [(i, i ^ distance) for i in range(count)])


def gathered(own, bits):
    pieces = [own]
    for _ in range(1, 1 << len(bits)):
        pieces.append(None)
    known = [0]
    for bit in bits:
        for offset in list(known):
            pieces[offset ^ bit] = swap(pieces[offset], "tp", bit)
            known.append(offset ^ bit)
    return pieces


def scattered(pieces, bits):
    sums = [piece.astype(F32) for piece in pieces]
    waiting = list(range(len(pieces)))
    for bit in bits:
        for offset in [other for other in waiting if other & bit]:
            outgoing = sums[offset].astype(BF16)
            moved = swap(outgoing, "tp", bit)
            rest = offset ^ bit
            sums[rest] = sums[rest] + moved.astype(F32)
        waiting = [other for other in waiting if not other & bit]
    return sums[0].astype(BF16)


def start_kernel(
    outer, inner, values, taps, document, mix_proj, local, edge, head, first_outer, *refs, count
):
    blocks = refs[: count + 1]
    fetched, kernel_rows, ids, shifted, seen, semaphores = refs[count + 1 :]
    length, channels = outer.shape
    half, width = blocks[0].shape
    core, own = lax.axis_index("sp") % 2, lax.axis_index("tp")
    plan = [
        (document, ids), (inner, fetched.at[0]), (values, fetched.at[1]), (outer, fetched.at[2]),
        (taps, kernel_rows),
    ]
    for index, block in enumerate(blocks):
        which, distance = (core, index) if index < count else (1 - core, 0)
        row = pl.multiple_of(which * half, half)
        column = pl.multiple_of((own ^ distance) * width, width)
        plan.append((mix_proj.at[pl.ds(row, half), pl.ds(column, width)], block))
    copies = [
        pltpu.make_async_copy(source, target, semaphores.at[place])
        for place, (source, target) in enumerate(plan)
    ]
    for copy in copies:
        copy.start()
    copies[0].wait()
    lanes = max(channels, 128)
    docs = jnp.broadcast_to(ids[...].astype(F32), (lanes, length)).T[:, :channels]
    seen[:8, :] = jnp.full((8, channels), -1.0, F32)
    seen[8:, :] = docs
    shifted[:8, :] = jnp.zeros((8, channels), F32)
    for copy in copies[1:5]:
        copy.wait()
    kernel = kernel_rows[...].astype(F32)
    product = fetched[0].astype(F32) * fetched[1].astype(F32)
    shifted[8:, :] = product
    conv = kernel[2:3] * product
    for back in (1, 2):
        window = slice(8 - back, 8 - back + length)
        same = seen[window, :] == docs
        conv = conv + kernel[2 - back : 3 - back] * jnp.where(same, shifted[window, :], 0.0)
    gate = fetched[2].astype(F32)
    local[...] = gate * conv
    first_outer[...] = gate[:8]
    head[...] = docs[:8]
    edge[:, :channels] = product[length - 8 :]
    edge[:, channels:] = docs[length - 8 :]
    for copy in copies[5:]:
        copy.wait()


def slot_kernel(routes, weights, spread, first, second, columns, *, groups, capacity):
    rows, length = first.shape
    place = lax.axis_index("sp")
    expert = lax.broadcasted_iota(jnp.int32, (groups, length), 0)
    named = [(routes[k : k + 1, :] == expert).astype(F32) for k in range(2)]
    earlier = lax.broadcasted_iota(jnp.int32, (length, length), 0)
    later = lax.broadcasted_iota(jnp.int32, (length, length), 1)
    before = jnp.dot(
        (named[0] + named[1]).astype(BF16),
        (earlier < later).astype(F32).astype(BF16),
        preferred_element_type=F32,
    )
    slot = lax.broadcasted_iota(jnp.int32, (rows, length), 0)
    total = jnp.zeros((rows, length), F32)
    for k, target in enumerate((first, second)):
        rank = jnp.sum(before * named[k], axis=0, keepdims=True).astype(jnp.int32)
        relative = routes[k : k + 1, :] ^ place
        block = (relative & 1) * (groups // 2) + (relative >> 1)
        chosen = (slot == block * capacity + rank).astype(F32)
        target[...] = chosen.astype(BF16)
        total = total + chosen
        columns[k] = jnp.broadcast_to(weights[k : k + 1, :], (128, length)).T
    spread[...] = total.astype(BF16)


def combine_kernel(total, first, second, columns, *refs, starts):
    landed, output = refs[:-1], refs[-1]
    result = total[...]
    for k, chosen in enumerate((first, second)):
        for block, start in zip(landed, starts):
            fetched = lax.dot_general(
                chosen[start : start + block.shape[0], :],
                block[...],
                (((0,), (0,)), ((), ())),
                preferred_element_type=F32,
            )
            result = result + fetched * columns[k][:, :1]
    output[...] = result.astype(output.dtype)


def edge_kernel(local, rim, head, first_outer, taps, gated):
    channels = local.shape[1]
    kernel = taps[...].astype(F32)
    older, newer = rim[6:7, :channels], rim[7:8, :channels]
    older_doc, newer_doc = rim[6:7, channels:], rim[7:8, channels:]
    doc = head[...]
    row = lax.broadcasted_iota(jnp.int32, doc.shape, 0)
    one = kernel[1:2] * jnp.where((row == 0) & (newer_doc == doc), newer, 0.0)
    two = kernel[0:1] * (
        jnp.where((row == 0) & (older_doc == doc), older, 0.0)
        + jnp.where((row == 1) & (newer_doc == doc), newer, 0.0)
    )
    gated[...] = local[...].astype(BF16)
    first = local[:16]
    fixed = jnp.concatenate([first[:8] + first_outer[...] * (one + two), first[8:]], axis=0)
    gated[:16, :] = fixed.astype(BF16)


def mix_kernel(stream, gain, spread, own_rest, rest, *refs, count):
    pieces, mine = refs[:count], refs[count : 2 * count]
    hidden, kept, given, weight = refs[2 * count :]
    half, width = own_rest.shape
    core = lax.axis_index("sp") % 2
    here = pl.ds(pl.multiple_of(core * half, half), half)
    there = pl.ds(pl.multiple_of((1 - core) * half, half), half)
    span = pl.ds(pl.multiple_of(lax.axis_index("tp") * width, width), width)
    total = stream[:, span].astype(F32)
    for index in range(count):
        weight[index, here, :] = mine[index][...]
        weight[index, there, :] = rest[index - 1] if index else own_rest[...]
        total = total + jnp.dot(
            pieces[index][...], weight[index], preferred_element_type=F32
        )
    hidden[...] = total
    scaled = (total * gain[:, span]).astype(BF16)
    rows = kept.shape[0]
    kept[...] = jnp.dot(spread[:rows], scaled, preferred_element_type=F32).astype(BF16)
    given[...] = jnp.dot(spread[rows:], scaled, preferred_element_type=F32).astype(BF16)


def expert_kernel(norm_gain, w_gate, w_up, w_down, *refs, count, block, epsilon):
    pieces, outputs, act = refs[:count], refs[count : 2 * count], refs[2 * count]
    own = lax.axis_index("tp")
    rows, width = pieces[0].shape
    spans = [
        pl.ds(pl.multiple_of((own ^ offset) * width, width), width) for offset in range(count)
    ]
    square = jnp.zeros((rows, 1), F32)
    for piece, span in zip(pieces, spans):
        value = piece[...].astype(F32) / norm_gain[:, span]
        square = square + jnp.sum(value * value, axis=1, keepdims=True)
    factor = lax.rsqrt(square / (count * width) + epsilon)
    for column in range(0, act.shape[1], block):
        both = []
        for table in (w_gate, w_up):
            total = jnp.zeros((rows, block), F32)
            for piece, span in zip(pieces, spans):
                total = total + jnp.dot(
                    piece[...],
                    table[0, span, column : column + block],
                    preferred_element_type=F32,
                )
            both.append(total * factor)
        gate, upper = both
        act[:, column : column + block] = (gate / (1.0 + jnp.exp(-gate)) * upper).astype(BF16)
    for output, span in zip(outputs, spans):
        output[...] = jnp.dot(
            act[...], w_down[0, :, span], preferred_element_type=F32
        ).astype(BF16)


def vmem_shape(shape, dtype):
    return pltpu.VMEM(tuple(shape), dtype)


def local_call(kernel, out_shape, scratch_shapes, arrays, flops=0):
    vmem = pl.BlockSpec(memory_space=pltpu.VMEM)
    return pl.pallas_call(
        kernel,
        in_specs=[vmem] * len(arrays),
        out_specs=[vmem] * len(out_shape) if isinstance(out_shape, list) else vmem,
        out_shape=out_shape,
        scratch_shapes=scratch_shapes,
        cost_estimate=pl.CostEstimate(flops=flops, bytes_accessed=0, transcendentals=0),
        compiler_params=pltpu.CompilerParams(vmem_limit_bytes=VMEM_LIMIT),
    )(*arrays)


def body(
    outer_gate,
    inner_gate,
    values,
    conv_taps,
    document,
    mix_proj,
    stream,
    norm_gain,
    routes,
    route_weight,
    w_gate,
    w_up,
    w_down,
):
    length, features = stream.shape
    groups = lax.axis_size("sp")
    parts = lax.axis_size("tp")
    capacity = 3 * length // groups
    chosen_count = routes.shape[1]
    width = features // parts
    chips = groups // 2
    channels = values.shape[1]
    bits = [1 << shift for shift in range(parts.bit_length() - 1)]

    half = channels // 2
    head_shape = vmem_shape((8, channels), F32)
    vmem = pl.BlockSpec(memory_space=pltpu.VMEM)
    local, edge, head, first_outer, *mine = pl.pallas_call(
        functools.partial(start_kernel, count=parts),
        in_specs=[pl.BlockSpec(memory_space=pltpu.HBM)] * 6,
        out_specs=[vmem] * (5 + parts),
        out_shape=[
            vmem_shape((length, channels), F32),
            vmem_shape((8, 2 * channels), F32),
            head_shape,
            head_shape,
        ]
        + [vmem_shape((half, width), BF16)] * (parts + 1),
        scratch_shapes=[
            pltpu.VMEM((3, length, channels), BF16),
            pltpu.VMEM(conv_taps.shape, BF16),
            pltpu.VMEM((1, length), jnp.int32),
            pltpu.VMEM((length + 8, channels), F32),
            pltpu.VMEM((length + 8, channels), F32),
            pltpu.SemaphoreType.DMA((6 + parts,)),
        ],
        compiler_params=pltpu.CompilerParams(vmem_limit_bytes=VMEM_LIMIT),
        cost_estimate=pl.CostEstimate(flops=10**10, bytes_accessed=1, transcendentals=0),
        name="start",
    )(
        *[
            pltpu.with_memory_space_constraint(array, pltpu.HBM)
            for array in (
                outer_gate, inner_gate, values, conv_taps, document.reshape(1, length), mix_proj
            )
        ],
    )
    own_rest = mine.pop()
    for distance in range(1, parts):
        mine[distance] = swap(mine[distance], "tp", distance)
    rim = lax.ppermute(edge, "sp", [(i, i + 1) for i in range(groups - 1)])
    rest = jnp.stack(mine[1:])
    rest = swap(rest, "sp", 1)
    gated = local_call(
        edge_kernel,
        vmem_shape((length, channels), BF16),
        [],
        [local, rim, head, first_outer, conv_taps],
    )
    pieces = [gated]
    for distance in range(1, parts):
        pieces.append(swap(gated, "tp", distance))

    rows = groups * capacity
    select = vmem_shape((rows, length), BF16)
    spread, first, second, columns = local_call(
        functools.partial(slot_kernel, groups=groups, capacity=capacity),
        [select, select, select, vmem_shape((chosen_count, length, 128), F32)],
        [],
        [routes.T, route_weight.T],
    )

    half_rows = chips * capacity
    hidden, kept, given = local_call(
        functools.partial(mix_kernel, count=parts),
        [
            vmem_shape((length, width), F32),
            vmem_shape((half_rows, width), BF16),
            vmem_shape((half_rows, width), BF16),
        ],
        [pltpu.VMEM((parts, channels, width), BF16)],
        [stream, norm_gain.reshape(1, features), spread, own_rest, rest, *pieces, *mine],
    )
    kept = kept.reshape(chips, capacity, width)
    mate = swap(given, "sp", 1).reshape(chips, capacity, width)

    quarter = chips // 4
    returned = [None] * chips
    gather_bits = [bits if order == "xy" else bits[::-1] for order in GATHERS]
    scatter_bits = [bits if order == "xy" else bits[::-1] for order in SCATTERS]
    for flow in range(4):
        members = list(range(flow * quarter, (flow + 1) * quarter))
        arrived = []
        for d in members:
            rows = jnp.concatenate([kept[d], mate[d]], axis=0)
            if d:
                rows = swap(rows, "sp", 2 * d)
            arrived.append(rows)
        pieces = gathered(jnp.concatenate(arrived, axis=0), gather_bits[flow])
        flow_rows = pieces[0].shape[0]
        outputs = local_call(
            functools.partial(
                expert_kernel,
                count=parts,
                block=min(512, w_gate.shape[2]),
                epsilon=1e-06,
            ),
            [vmem_shape((flow_rows, width), BF16)] * parts,
            [pltpu.VMEM((flow_rows, w_gate.shape[2]), BF16)],
            [norm_gain.reshape(1, features), w_gate, w_up, w_down, *pieces],
            6 * flow_rows * features * w_gate.shape[2],
        )
        total = scattered(outputs, scatter_bits[flow])
        total = total.reshape(len(members), 2 * capacity, width)
        for index, d in enumerate(members):
            back = total[index]
            if d:
                back = swap(back, "sp", 2 * d)
            returned[d] = back
    total = hidden
    for name, members in (("bs", range(1, chips)), ("bo", range(1))):
        here = jnp.concatenate([returned[d][:capacity] for d in members], axis=0)
        there = jnp.concatenate([returned[d][capacity:] for d in members], axis=0)
        there = swap(there, "sp", 1)
        final = name == "bo"
        start = members[0] * capacity
        total = local_call(
            functools.partial(combine_kernel, starts=(start, half_rows + start)),
            jax.ShapeDtypeStruct((length, width), BF16)
            if final
            else vmem_shape((length, width), F32),
            [],
            [total, first, second, columns, here, there],
        )
    return total


def solution(mesh):
    return jax.shard_map(
        body,
        mesh=mesh,
        in_specs=(
            P("sp", "tp"),
            P("sp", "tp"),
            P("sp", "tp"),
            P(None, "tp"),
            P("sp"),
            P("tp", None),
            P("sp", None),
            P(),
            P("sp", None),
            P("sp", None),
            P("sp", None, "tp"),
            P("sp", None, "tp"),
            P("sp", "tp", None),
        ),
        out_specs=P("sp", "tp"),
        check_vma=False,
    )
```
